32 devices in a mesh: ep: 8 (over z, x), tp: 4 (over y, core).
Axes of the slice: x: 2, y: 2, z: 4, core: 2. Of those that a mesh axis runs over, the one named last changes fastest.
Arguments:
- tokens: bfloat16 [2048, 2048], P('ep'), may hold values from -40 to 40
- cotangent: bfloat16 [2048, 2048], P('ep'), may hold values from -6 to 6
- expert_ids: int32 [2048, 4], P('ep'), may hold values from 0 to 15, all different within a row; in each aligned block of 256 rows (0 to 255, 256 to 511, ...) at most 96 rows name the same one
- route_weights: bfloat16 [2048, 4], P('ep'), may hold values from 0.099609375 to 1
- gate_weight: bfloat16 [16, 2048, 2048], P('ep', None, 'tp'), may hold values from -0.125 to 0.125
- up_weight: bfloat16 [16, 2048, 2048], P('ep', None, 'tp'), may hold values from -0.125 to 0.125
- down_weight: bfloat16 [16, 2048, 2048], P('ep', 'tp'), may hold values from -0.125 to 0.125
- dense_weight: bfloat16 [2048, 2048], P('tp', 'ep'), may hold values from -0.125 to 0.125
- dense_gate: float32 [2048], replicated, may hold values from 0.1 to 1.9
Outputs:
- token_grad: bfloat16 [2048, 2048], P('ep', 'tp')
- weight_grad: bfloat16 [2048, 4], P('ep')
- gate_grad: float32 [16, 2048, 2048], P('ep', None, 'tp')
- up_grad: float32 [16, 2048, 2048], P('ep', None, 'tp')
- down_grad: float32 [16, 2048, 2048], P('ep', 'tp')
- dense_grad: float32 [2048, 2048], P('tp', 'ep')
The draws below stay inside these ranges and needn't reach their ends.
Inputs may be any that keep to these rules, and one draw needn't show every extreme that they name: `expert_ids`: in the rows of one device, at most 96 routed rows name any one expert, and in every draw some expert is named by exactly 96 rows of some device.
All inputs are finite; a program needn't handle non-finite values.
Results may differ from the reference program's by a relative error of at most 0.02.
Values may be sent and summed in bfloat16 or wider, within the bound.
No kernel may reach another device: no remote copies, remote signals or barrier semaphores. Data moves between devices by JAX's collectives and lax.ppermute only.
A program may use at most 128 MiB of HBM per device.

```python
import math
import jax
import jax.numpy as jnp
import numpy as np
from jax import lax

D = 2048
FF = 2048
TOP_K = 4
TOK_DEV = 256
EXPERTS = 16
TOKENS = 2048
CAP = 96
N_EP = 8
N_TP = 4


def draw_tokens(key, part):
    key_scale = jax.random.fold_in(key, 11)
    key_base = jax.random.fold_in(key, 12)
    row_scale = jnp.exp(jax.random.uniform(key_scale, (TOKENS, 1), jnp.float32, math.log(0.5), math.log(6.0)))
    values = jax.random.normal(key_base, (TOKENS, D), jnp.float32)
    return jnp.clip(values * row_scale, -40.0, 40.0).astype(jnp.bfloat16)


def with_spikes(result, stream_key, source, target, blocks, factor):
    def block_of(axis_at):
        return (jnp.arange(result.shape[axis_at]) // (result.shape[axis_at] // blocks)).reshape((-1,) + (1,) * (result.ndim - 1 - axis_at))

    first = jax.random.permutation(stream_key, blocks)[block_of(target)]
    second = (block_of(target) + blocks // 2) % blocks
    return jnp.where((block_of(source) == first) | (block_of(source) == second), factor * result, result)


def block_levels(own_key, shape, cuts, least, top_value):
    level = 1.0
    for dim, blocks in cuts:
        steps = jax.random.uniform(jax.random.fold_in(jax.random.fold_in(own_key, 6), dim), (blocks,), jnp.float32, least / len(cuts), top_value / len(cuts))
        level = level * jnp.repeat(jnp.exp(steps), shape[dim] // blocks).reshape((-1,) + (1,) * (len(shape) - 1 - dim))
    return level


def routed_block(key, own, number, rows, number_of, top, bound, lean):
    sequence = jax.random.permutation(key, number_of)
    heavy_load, common = load_shares(number_of, rows * top, bound, lean, True), load_shares(number_of, rows * top, bound, lean, False)
    places = jnp.arange(number_of)

    def named(tallies, offset_by):
        used = int((tallies > 0).sum())
        fixed = max(1, used // 4)
        moved = fixed + (places - fixed + offset_by * (used - fixed)) % max(1, number_of - fixed)
        return jnp.zeros((number_of,), jnp.int32).at[sequence[jnp.where(places < fixed, places, moved)]].set(jnp.asarray(tallies, jnp.int32))

    tallies = jnp.where(number % 4 == 0, named(heavy_load, number // 4), named(common, number - number // 4 - 1))
    mixed = jax.random.permutation(jax.random.fold_in(own, 3), number_of)
    source_of, taker = mixed[0:number_of // 2 * 2:2], mixed[1:number_of // 2 * 2:2]
    margin = jnp.minimum(tallies[source_of] - 1, bound - tallies[taker]) // 2
    margin = jnp.where((source_of == sequence[0]) | (taker == sequence[0]) | (tallies[taker] == 0), 0, jnp.maximum(margin, 0))
    moved = jax.random.randint(jax.random.fold_in(own, 4), (number_of // 2,), 0, 1 << 20) % (margin + 1)
    tallies = tallies.at[source_of].add(-moved).at[taker].add(moved)
    labels = jnp.searchsorted(jnp.cumsum(tallies), jnp.arange(rows * top), side="right").astype(jnp.int32)
    listing = labels.reshape(top, rows).T
    listing = listing[jax.random.permutation(jax.random.fold_in(own, 1), rows)]
    offset_by = jax.random.randint(jax.random.fold_in(own, 2), (rows, 1), 0, top)
    return jnp.take_along_axis(listing, (jnp.arange(top)[None, :] + offset_by) % top, axis=1)


def load_shares(count, total, most, skew, full):
    loads = [(1 << 20) // math.isqrt(grade ** skew) + 1 for grade in range(1, count + 1)]
    largest = most if full else min(most, max(-(-total // count), total * loads[0] // sum(loads)))
    least = 1 if total - largest >= count - 1 else 0
    given, surplus = [largest] + [least] * (count - 1), total - largest - least * (count - 1)
    while surplus > 0:
        candidates = [i for i in range(1, count) if given[i] < largest] or [i for i in range(1, count) if given[i] < most]
        whole, remaining = sum([loads[i] for i in candidates]), surplus
        for i in candidates:
            extra = min(most - given[i], max(1, remaining * loads[i] // whole), surplus)
            given[i] = given[i] + extra
            surplus = surplus - extra
    return np.array(given)


def noise(own_key, extent, width, limit, cuts=(), kind=jnp.bfloat16):
    result = width * jax.random.normal(own_key, extent, jnp.float32)
    if cuts:
        result = result * block_levels(own_key, extent, cuts, -0.22, 0.18)
    return jnp.clip(result, -limit, limit).astype(kind)


def gaussian_with(own_key, shape, deviation, most, cuts, heavy, kind=jnp.bfloat16):
    result = deviation * jax.random.normal(own_key, shape, jnp.float32)
    if cuts:
        result = result * block_levels(own_key, shape, cuts, -0.22, 0.18)
    return jnp.clip(with_spikes(result, jax.random.fold_in(own_key, 3), *heavy), -most, most).astype(kind)


def setup_inputs(seed: int = 0) -> dict:
    splits = jax.random.split(jax.random.key(seed), 10)
    tokens = draw_tokens(jax.random.fold_in(splits[9], 71), 0)
    cotangent = gaussian_with(splits[1], (TOKENS, D), 1.0, 6.0, ((0, 8),), (0, 1, 8, 2.0))
    expert_ids_keys = jax.random.split(jax.random.fold_in(splits[2], 1), TOKENS // TOK_DEV)
    expert_ids_turns = jax.random.permutation(jax.random.fold_in(splits[2], 3), TOKENS // TOK_DEV)
    expert_ids = jax.vmap(lambda own, number: routed_block(jax.random.fold_in(splits[2], 2), own, number, TOK_DEV, EXPERTS, TOP_K, CAP, 2))(expert_ids_keys, expert_ids_turns).reshape((TOKENS, TOP_K))
    route_weights = jnp.clip(0.099609375 + 0.9003906 * jax.random.uniform(splits[3], (TOKENS, TOP_K), jnp.float32) ** block_levels(splits[3], (TOKENS, TOP_K), ((0, 8),), -0.2, 0.2), 0.099609375, 1.0).astype(jnp.bfloat16)
    gate_weight = noise(splits[4], (EXPERTS, D, FF), D ** -0.5, 0.125, ((0, 8), (2, 4)))
    up_weight = noise(splits[5], (EXPERTS, D, FF), D ** -0.5, 0.125, ((0, 8), (2, 4)))
    down_weight = noise(splits[6], (EXPERTS, FF, D), FF ** -0.5, 0.125, ((0, 8), (1, 4)))
    dense_weight = noise(splits[7], (D, D), D ** -0.5, 0.125, ((0, 4), (1, 8)))
    dense_gate = jnp.clip(1.0 + 0.18 * jax.random.normal(splits[8], (D,), jnp.float32), 0.1, 1.9)
    return dict(tokens=tokens, cotangent=cotangent, expert_ids=expert_ids, route_weights=route_weights, gate_weight=gate_weight, up_weight=up_weight, down_weight=down_weight, dense_weight=dense_weight, dense_gate=dense_gate)


clamp_limit = 7.0
sigmoid_slope = 1.702


def rounded(value):
    return lax.optimization_barrier(value.astype(jnp.bfloat16)).astype(jnp.float32)


def expert_back(row_input, row_cotan, row_weight, w_gate, w_up, w_down):
    gate_pre = jnp.dot(row_input, w_gate, preferred_element_type=jnp.float32)
    up_pre = jnp.dot(row_input, w_up, preferred_element_type=jnp.float32)
    gate_val = jnp.minimum(gate_pre, clamp_limit)
    up_val = jnp.clip(up_pre, -clamp_limit, clamp_limit)
    squash = jax.nn.sigmoid(sigmoid_slope * gate_val)
    hidden = ((up_val + 1.0) * gate_val * squash).astype(jnp.bfloat16)
    down_back = lax.dot_general(row_cotan, w_down, (((1,), (1,)), ((), ())), preferred_element_type=jnp.float32)
    scores = jnp.sum(hidden.astype(jnp.float32) * down_back, axis=1)
    scale_col = row_weight.astype(jnp.float32)[:, None]
    hidden_back = scale_col * down_back
    gate_slope = squash + sigmoid_slope * gate_val * squash * (1.0 - squash)
    gate_back = jnp.where(gate_pre < clamp_limit, hidden_back * (up_val + 1.0) * gate_slope, 0.0).astype(jnp.bfloat16)
    up_back = jnp.where(jnp.abs(up_pre) < clamp_limit, hidden_back * gate_val * squash, 0.0).astype(jnp.bfloat16)
    weighted = (scale_col * row_cotan.astype(jnp.float32)).astype(jnp.bfloat16)
    input_back = lax.dot_general(gate_back, w_gate, (((1,), (1,)), ((), ())), preferred_element_type=jnp.float32)
    input_back = input_back + lax.dot_general(up_back, w_up, (((1,), (1,)), ((), ())), preferred_element_type=jnp.float32)
    grad_gate = lax.dot_general(row_input, gate_back, (((0,), (0,)), ((), ())), preferred_element_type=jnp.float32)
    grad_up = lax.dot_general(row_input, up_back, (((0,), (0,)), ((), ())), preferred_element_type=jnp.float32)
    grad_down = lax.dot_general(hidden, weighted, (((0,), (0,)), ((), ())), preferred_element_type=jnp.float32)
    return input_back, scores, grad_gate, grad_up, grad_down


def reference(tokens, cotangent, expert_ids, route_weights, gate_weight, up_weight, down_weight, dense_weight, dense_gate):
    routed = TOKENS * TOP_K
    flat_ids = expert_ids.reshape(routed).astype(jnp.int32)
    sorted_rows = jnp.argsort(flat_ids, stable=True).astype(jnp.int32)
    onehot = (flat_ids[:, None] == jnp.arange(EXPERTS, dtype=jnp.int32)[None, :]).astype(jnp.int32)
    counts = jnp.sum(onehot, axis=0).astype(jnp.int32)
    starts = (jnp.cumsum(counts) - counts).astype(jnp.int32)
    longest = N_EP * CAP
    flat_weights = route_weights.reshape(routed)
    unit_block = FF // N_TP

    def one_expert(expert):
        offsets = jnp.arange(longest, dtype=jnp.int32)
        in_use = offsets < counts[expert]
        row_ids = sorted_rows[jnp.minimum(starts[expert] + offsets, routed - 1)]
        owners = (row_ids // TOP_K).astype(jnp.int32)
        bf_zero = jnp.zeros((), jnp.bfloat16)
        row_input = jnp.where(in_use[:, None], tokens[owners], bf_zero)
        row_cotan = jnp.where(in_use[:, None], cotangent[owners], bf_zero)
        row_weight = jnp.where(in_use, flat_weights[row_ids], bf_zero)
        back_sum = jnp.zeros((longest, D), jnp.float32)
        score_sum = jnp.zeros((longest,), jnp.float32)
        gate_parts, up_parts, down_parts = [], [], []
        for segment in range(N_TP):
            low = segment * unit_block
            high = low + unit_block
            pieces_out = expert_back(row_input, row_cotan, row_weight, gate_weight[expert][:, low:high],
                                     up_weight[expert][:, low:high], down_weight[expert][low:high, :])
            back_sum = back_sum + rounded(pieces_out[0])
            score_sum = score_sum + rounded(pieces_out[1])
            gate_parts.append(pieces_out[2])
            up_parts.append(pieces_out[3])
            down_parts.append(pieces_out[4])
        targets = jnp.where(in_use, row_ids, routed).astype(jnp.int32)
        return (back_sum.astype(jnp.bfloat16), score_sum, targets, jnp.concatenate(gate_parts, axis=1),
                jnp.concatenate(up_parts, axis=1), jnp.concatenate(down_parts, axis=0))

    backs, scores, targets, gate_grad, up_grad, down_grad = lax.map(one_expert, jnp.arange(EXPERTS, dtype=jnp.int32))
    flat_targets = targets.reshape(EXPERTS * longest)
    flat_back = jnp.zeros((routed + 1, D), jnp.float32).at[flat_targets].add(backs.reshape(EXPERTS * longest, D).astype(jnp.float32))
    flat_score = jnp.zeros((routed + 1,), jnp.float32).at[flat_targets].add(scores.reshape(EXPERTS * longest))
    gated_cotan = (dense_gate[None, :] * cotangent.astype(jnp.float32)).astype(jnp.bfloat16)
    dense_back = lax.dot_general(gated_cotan, dense_weight, (((1,), (1,)), ((), ())), preferred_element_type=jnp.float32)
    dense_grad = lax.dot_general(tokens, gated_cotan, (((0,), (0,)), ((), ())), preferred_element_type=jnp.float32)
    token_grad = (jnp.sum(flat_back[:routed].reshape(TOKENS, TOP_K, D), axis=1) + dense_back).astype(jnp.bfloat16)
    weight_grad = flat_score[:routed].reshape(TOKENS, TOP_K).astype(jnp.bfloat16)
    return token_grad, weight_grad, gate_grad, up_grad, down_grad, dense_grad
```

```python
import functools

import jax
import jax.numpy as jnp
from jax import lax
from jax.experimental import pallas as pl
from jax.experimental.pallas import tpu as pltpu
from jax.sharding import PartitionSpec as P


clamp_limit = 7.0
sigmoid_slope = 1.702
f32, bf16 = jnp.float32, jnp.bfloat16


def swap(value, axis, mask):
    size = lax.axis_size(axis)
    return lax.ppermute(value, axis, [(i, i ^ mask) for i in range(size)])


def columns(lhs, rhs):
    return lax.dot_general(lhs, rhs, (((1,), (1,)), ((), ())), preferred_element_type=f32)


def outer(lhs, rhs):
    return lax.dot_general(lhs, rhs, (((0,), (0,)), ((), ())), preferred_element_type=f32)


def pair_kernel(layout, local, cap, *refs):
    count = len(layout)
    inputs, refs = refs[: sum(n for n, _ in layout)], refs[sum(n for n, _ in layout) :]
    stored, (dense_w_ref, dense_g_ref, dgrad_in) = refs[:3], refs[3:6]
    held, (weight_sems, block, meta, picks, rows_s, cots_s, back, dense, score_total, sems) = (
        refs[-13:-10], refs[-10:]
    )
    wg_ref, wu_ref, wd_ref = held
    row_ref, hid_ref, gb_ref, ub_ref, wt_ref, keep_ref, send_ref, dgrad_ref = refs[-21:-13]
    tp, ep, e = lax.axis_index("tp"), lax.axis_index("ep"), pl.program_id(0)
    tp_size = lax.axis_size("tp")
    tok_rows, width = block.shape[2:]

    def weight_copy(i, j):
        return pltpu.make_async_copy(stored[i].at[j], held[i].at[j], weight_sems.at[i, j])

    top = meta.shape[1] // 2
    step = min(512, width)

    def table(b, expert):
        values = meta[b].astype(f32)
        match = (values[:top] == expert.astype(f32)).astype(f32)
        return (
            match,
            jnp.sum(match, axis=0, keepdims=True),
            jnp.sum(match * values[top:], axis=0, keepdims=True),
        )

    @pl.when(e == 0)
    def _():
        copies, counts, n = [], [0], 0

        def fetch(source, target):
            copy = pltpu.make_async_copy(source, target, sems.at[len(copies)])
            copy.start()
            copies.append(copy)

        for b, (number, masks) in enumerate(layout):
            mine = inputs[n : n + number]
            n += number
            if masks is None:
                fetch(mine[0], block.at[b, 0])
                fetch(mine[1], block.at[b, 1])
                fetch(mine[2], meta.at[b])
                counts.append(len(copies))
                continue
            for i, (piece, mask) in enumerate(zip(mine, masks)):
                rows = (piece.shape[0] - 2 * top) // 2
                other = tp ^ mask
                if rows * 2 == tok_rows:
                    place = (other % 2) * rows
                else:
                    place = ((other % 2) * (tp_size // 2) + other // 2) * rows
                place = pl.ds(pl.multiple_of(place, 16), rows)
                fetch(piece.at[:rows], block.at[b, 0, place])
                fetch(piece.at[rows : 2 * rows], block.at[b, 1, place])
                if i == 0:
                    fetch(piece.at[2 * rows :, :tok_rows], meta.at[b])
            counts.append(len(copies))
        for j in range(local):
            for i in range(3):
                weight_copy(i, j).start()
        before = (
            lax.broadcasted_iota(jnp.int32, (tok_rows, tok_rows), 0)
            < lax.broadcasted_iota(jnp.int32, (tok_rows, tok_rows), 1)
        )
        before = jnp.where(before, 1.0, 0.0).astype(bf16)
        slot = lax.broadcasted_iota(jnp.int32, (cap, tok_rows), 0).astype(f32)
        out_part, in_part = dense_w_ref.shape[1], dense_w_ref.shape[0]
        own_cols = pl.ds(pl.multiple_of(tp * in_part, 128), in_part)
        out_cols = pl.ds(pl.multiple_of(ep * out_part, 128), out_part)
        dense_sum = dgrad_in[...]
        for b in range(count):
            for copy in copies[counts[b] : counts[b + 1]]:
                copy.wait()
            for j in range(local):
                chosen = table(b, ep * local + j)[1]
                rank = jnp.dot(
                    jnp.broadcast_to(chosen, (8, tok_rows)).astype(bf16),
                    before,
                    preferred_element_type=f32,
                )[:1]
                place = jnp.where(chosen > 0.0, rank, -1.0)
                picks[b, j * cap : (j + 1) * cap] = jnp.where(slot == place, 1.0, 0.0).astype(bf16)
            for which, out in ((0, rows_s), (1, cots_s)):
                for low in range(0, width, step):
                    got = jnp.dot(
                        picks[b], block[b, which, :, low : low + step],
                        preferred_element_type=f32,
                    ).astype(bf16)
                    for j in range(local):
                        out[j, b * cap : (b + 1) * cap, low : low + step] = got[
                            j * cap : (j + 1) * cap
                        ]
            gated = (dense_g_ref[:, out_cols] * block[b, 1, :, out_cols].astype(f32)).astype(bf16)
            dense[b] = columns(gated, dense_w_ref[...])
            dense_sum = dense_sum + outer(block[b, 0, :, own_cols], gated)
        dgrad_ref[...] = dense_sum
        score_total[...] = jnp.zeros_like(score_total)

    for i in range(3):
        weight_copy(i, e).wait()
    rows, cots = rows_s[e], cots_s[e]
    row_ref[0] = rows
    own_rows = pl.ds(pl.multiple_of(e * cap, 16), cap)
    own_picks = [picks[b, own_rows] for b in range(count)]
    tables = [table(b, ep * local + e) for b in range(count)]
    scale = jnp.concatenate(
        [
            jnp.sum(own_picks[b].astype(f32) * tables[b][2], axis=1, keepdims=True)
            for b in range(count)
        ],
        axis=0,
    )
    gate_pre = jnp.dot(rows, wg_ref[e], preferred_element_type=f32)
    up_pre = jnp.dot(rows, wu_ref[e], preferred_element_type=f32)
    down_back = columns(cots, wd_ref[e])
    gate_val = jnp.minimum(gate_pre, clamp_limit)
    up_val = jnp.clip(up_pre, -clamp_limit, clamp_limit)
    squash = jax.nn.sigmoid(sigmoid_slope * gate_val)
    hidden = ((up_val + 1.0) * gate_val * squash).astype(bf16)
    product = hidden.astype(f32) * down_back
    hidden_back = scale * down_back
    gate_slope = squash + sigmoid_slope * gate_val * squash * (1.0 - squash)
    gate_back = jnp.where(
        gate_pre < clamp_limit, hidden_back * (up_val + 1.0) * gate_slope, 0.0
    ).astype(bf16)
    up_back = jnp.where(
        jnp.abs(up_pre) < clamp_limit, hidden_back * gate_val * squash, 0.0
    ).astype(bf16)
    hid_ref[0], gb_ref[0], ub_ref[0] = hidden, gate_back, up_back
    wt_ref[0] = (scale * cots.astype(f32)).astype(bf16)
    for low in range(0, width, step):
        cols = slice(low, low + step)
        value = (
            columns(gate_back, wg_ref[e, cols]) + columns(up_back, wu_ref[e, cols])
        ).astype(bf16)
        for b in range(count):
            back[b, own_rows, cols] = value[b * cap : (b + 1) * cap]
    score = jnp.sum(product, axis=1, keepdims=True)
    for b in range(count):
        by_token = jnp.sum(
            own_picks[b].astype(f32) * score[b * cap : (b + 1) * cap], axis=0, keepdims=True
        )
        score_total[b, :top] += tables[b][0] * by_token

    @pl.when(e == local - 1)
    def _():
        part = dense.shape[2]
        for b in range(count):
            for p in range(tp_size):
                out = send_ref if p % 2 else keep_ref
                cols = pl.ds(pl.multiple_of((tp ^ p) * part, 128), part)
                value = outer(picks[b], back[b, :, cols])
                if p == 0:
                    value = value + dense[b]
                out[b, p // 2, :tok_rows] = value.astype(bf16)
                out[b, p // 2, tok_rows:] = jnp.zeros((out.shape[2] - tok_rows, part), bf16)
                out[b, p // 2, tok_rows:, :tok_rows] = score_total[b].astype(bf16)


def expert_pair(
    blocks, weights, dense_w, dense_g, dgrad, slabs, index, count_all, tok_rows, cap, top
):
    local, width, units = weights[0].shape
    count = len(blocks)
    part = dense_w.shape[0]
    halves = lax.axis_size("tp") // 2
    m = count * cap
    vmem = pl.BlockSpec(memory_space=pltpu.VMEM)
    hbm = pl.BlockSpec(memory_space=pltpu.HBM)
    arrays = [v for values, _ in blocks for v in values]
    layout = tuple((len(values), masks) for values, masks in blocks)
    payload = jax.ShapeDtypeStruct((count, halves, tok_rows + 8, part), bf16)
    window = lambda lanes: pl.BlockSpec((1, m, lanes), lambda e: (e, index, 0))
    slab_lanes = (width, units, units, units, width)
    operands = [*arrays, *weights, dense_w, dense_g, dgrad]
    specs = [hbm] * (len(arrays) + 3) + [vmem] * 3
    aliases = {}
    if slabs is not None:
        aliases = {len(operands) + i: i for i in range(5)}
        operands += list(slabs)
        specs += [hbm] * 5
    return pl.pallas_call(
        functools.partial(pair_kernel, layout, local, cap),
        grid=(local,),
        out_shape=(
            *[jax.ShapeDtypeStruct((local, count_all * m, n), bf16) for n in slab_lanes],
            payload,
            payload,
            jax.ShapeDtypeStruct(dgrad.shape, f32),
        ),
        in_specs=specs,
        out_specs=(*[window(n) for n in slab_lanes], vmem, vmem, vmem),
        scratch_shapes=[
            *[pltpu.VMEM(w.shape, bf16) for w in weights],
            pltpu.SemaphoreType.DMA((3, local)),
            pltpu.VMEM((count, 2, tok_rows, width), bf16),
            pltpu.VMEM((count, 2 * top, tok_rows), bf16),
            pltpu.VMEM((count, local * cap, tok_rows), bf16),
            pltpu.VMEM((local, m, width), bf16),
            pltpu.VMEM((local, m, width), bf16),
            pltpu.VMEM((count, local * cap, width), bf16),
            pltpu.VMEM((count, tok_rows, part), f32),
            pltpu.VMEM((count, 8, tok_rows), f32),
            pltpu.SemaphoreType.DMA((3 * len(arrays),)),
        ],
        input_output_aliases=aliases,
        compiler_params=pltpu.CompilerParams(vmem_limit_bytes=56 << 20),
        cost_estimate=pl.CostEstimate(
            flops=14 * local * m * width * units,
            bytes_accessed=10 * local * width * units,
            transcendentals=local * m * units,
        ),
        name="expert_pair",
    )(*operands)


def batched(lhs, rhs):
    return lax.dot_general(lhs, rhs, (((1,), (1,)), ((0,), (0,))), preferred_element_type=f32)


def shards(
    tokens,
    cotangent,
    expert_ids,
    route_weights,
    gate_weight,
    up_weight,
    down_weight,
    dense_weight,
    dense_gate,
):
    tok_rows, width = tokens.shape
    top_count = expert_ids.shape[1]
    local = gate_weight.shape[0]
    ep_size = lax.axis_size("ep")
    tp_size = lax.axis_size("tp")
    ep, tp = lax.axis_index("ep"), lax.axis_index("tp")
    cap = tok_rows * top_count * 3 // (2 * local * ep_size)
    halves = tp_size // 2
    quarter_rows = tok_rows // tp_size
    half_rows = tok_rows // 2

    meta = jnp.concatenate([expert_ids.T.astype(bf16), route_weights.T], axis=0)
    meta_rows = jnp.pad(meta, ((0, 0), (0, width - tok_rows)))

    def share(start, rows):
        return jnp.concatenate(
            [
                lax.dynamic_slice_in_dim(tokens, start, rows, 0),
                lax.dynamic_slice_in_dim(cotangent, start, rows, 0),
                meta_rows,
            ],
            axis=0,
        )

    own_half = share((tp % 2) * half_rows, half_rows)
    own_quarter = share(((tp % 2) * halves + tp // 2) * quarter_rows, quarter_rows)
    pairs = ep_size // 2
    line = pairs == 4 and halves == 2
    middle = (ep // 2 == 1) | (ep // 2 == 2)

    def along(value, moves):
        return lax.ppermute(
            value, "ep", [(2 * a + i, 2 * b + i) for a, b in moves for i in range(2)]
        )

    far = [None] * pairs
    if line:
        far[1] = along(own_quarter, ((0, 1), (1, 0), (2, 3), (3, 2)))
        inner = along(own_quarter, ((1, 2), (2, 1)))
        far[2] = jnp.where(middle, inner, along(inner, ((1, 0), (2, 3))))
        inner = along(far[1], ((1, 2), (2, 1)))
        far[3] = jnp.where(middle, inner, along(inner, ((1, 0), (2, 3))))
    else:
        for k in range(1, pairs):
            far[k] = swap(own_quarter, "ep", 2 * k)
    near = [swap(own_half, "ep", 1)]
    near += [swap(far[k], "ep", 1) for k in range(1, pairs)]

    def gathered(value, whole):
        held = [(value, 0)]
        if not whole:
            held += [(swap(value, "tp", 2 * p), 2 * p) for p in range(1, halves)]
        held += [(swap(v, "tp", 1), mask ^ 1) for v, mask in tuple(held)]
        return [v for v, _ in held], tuple(mask for _, mask in held)

    blocks = [[([tokens, cotangent, meta], None), gathered(near[0], True)]]
    for k in range(1, pairs):
        blocks.append([gathered(far[k], False), gathered(near[k], False)])

    dense_g = dense_gate[None, :]
    dgrad = jnp.zeros(dense_weight.shape, f32)
    weights = (gate_weight, up_weight, down_weight)
    slabs = None
    results = {}
    for k in range(pairs):
        *slabs, keep, send, dgrad = expert_pair(
            blocks[k], weights, dense_weight, dense_g, dgrad, slabs, k, pairs, tok_rows, cap,
            top_count,
        )
        other = swap(send, "tp", 1)
        both = keep.astype(f32) + other.astype(f32)
        moved = swap(both[1].astype(bf16), "ep", 1)
        both = both[0] + moved.astype(f32)
        total = both[0]
        for h in range(1, halves):
            total = total + swap(both[h].astype(bf16), "tp", 2 * h).astype(f32)
        results[k] = total
    row, hid, gb, ub, wt = slabs
    grads = []
    for left, right in ((row, gb), (row, ub), (hid, wt)):
        grads.append(batched(left, right))
    grad_gate, grad_up, grad_down = grads

    total = results[0]
    for k in range(1, pairs):
        value = results[k].astype(bf16)
        if not line or k == 1:
            total = total + swap(value, "ep", 2 * k).astype(f32)
            continue
        straight, crossed = ((0, 2), (3, 1)), ((1, 2), (2, 1))
        if k == 3:
            straight, crossed = ((1, 3), (2, 0)), ((0, 3), (3, 0))
        total = total + along(value, straight).astype(f32)
        total = total + along(value, crossed).astype(f32)
    token_grad = total[:tok_rows].astype(bf16)
    weight_grad = total[tok_rows : tok_rows + top_count, :tok_rows].astype(bf16).T
    return (token_grad, weight_grad, grad_gate, grad_up, grad_down, dgrad)


def solution(mesh):
    in_specs = (
        P("ep", None),
        P("ep", None),
        P("ep", None),
        P("ep", None),
        P("ep", None, "tp"),
        P("ep", None, "tp"),
        P("ep", "tp", None),
        P("tp", "ep"),
        P(),
    )
    out_specs = (
        P("ep", "tp"),
        P("ep", None),
        P("ep", None, "tp"),
        P("ep", None, "tp"),
        P("ep", "tp", None),
        P("tp", "ep"),
    )

    return jax.shard_map(shards, mesh=mesh, in_specs=in_specs, out_specs=out_specs, check_vma=False)
```

```python
import functools

import jax
import jax.numpy as jnp
from jax import lax
from jax.experimental import pallas as pl
from jax.experimental.pallas import tpu as pltpu
from jax.sharding import PartitionSpec as P


clamp_limit = 7.0
sigmoid_slope = 1.702
f32, bf16 = jnp.float32, jnp.bfloat16


def swap(value, axis, mask):
    size = lax.axis_size(axis)
    return lax.ppermute(value, axis, [(i, i ^ mask) for i in range(size)])


def columns(lhs, rhs):
    return lax.dot_general(lhs, rhs, (((1,), (1,)), ((), ())), preferred_element_type=f32)


def outer(lhs, rhs):
    return lax.dot_general(lhs, rhs, (((0,), (0,)), ((), ())), preferred_element_type=f32)


def pair_kernel(layout, local, cap, fresh, *refs):
    count = len(layout)
    inputs, refs = refs[: sum(n for n, _ in layout)], refs[sum(n for n, _ in layout) :]
    stored, (dense_w_ref, dense_g_ref) = refs[:3], refs[3:5]
    dgrad_in = None if fresh else refs[5]
    held, (weight_sems, block, meta, picks, rows_s, cots_s, back, dense, score_total, sems) = (
        refs[-13:-10], refs[-10:]
    )
    wg_ref, wu_ref, wd_ref = held
    row_ref, hid_ref, gb_ref, ub_ref, wt_ref, keep_ref, send_ref, dgrad_ref = refs[-21:-13]
    tp, ep, e = lax.axis_index("tp"), lax.axis_index("ep"), pl.program_id(0)
    tp_size = lax.axis_size("tp")
    tok_rows, width = block.shape[2:]

    def weight_copy(i, j):
        return pltpu.make_async_copy(stored[i].at[j], held[i].at[j], weight_sems.at[i, j])

    top = meta.shape[1] // 2
    step = min(512, width)

    def table(b, expert):
        values = meta[b].astype(f32)
        match = (values[:top] == expert.astype(f32)).astype(f32)
        return (
            match,
            jnp.sum(match, axis=0, keepdims=True),
            jnp.sum(match * values[top:], axis=0, keepdims=True),
        )

    @pl.when(e == 0)
    def _():
        copies, counts, n = [], [0], 0

        def fetch(source, target):
            copy = pltpu.make_async_copy(source, target, sems.at[len(copies)])
            copy.start()
            copies.append(copy)

        for b, (number, masks) in enumerate(layout):
            mine = inputs[n : n + number]
            n += number
            if masks is None:
                fetch(mine[0], block.at[b, 0])
                fetch(mine[1], block.at[b, 1])
                fetch(mine[2], meta.at[b])
                counts.append(len(copies))
                continue
            for i, (piece, mask) in enumerate(zip(mine, masks)):
                rows = (piece.shape[0] - 2 * top) // 2
                other = tp ^ mask
                if rows * 2 == tok_rows:
                    place = (other % 2) * rows
                else:
                    place = ((other % 2) * (tp_size // 2) + other // 2) * rows
                place = pl.ds(pl.multiple_of(place, 16), rows)
                fetch(piece.at[:rows], block.at[b, 0, place])
                fetch(piece.at[rows : 2 * rows], block.at[b, 1, place])
                if i == 0:
                    fetch(piece.at[2 * rows :, :tok_rows], meta.at[b])
            counts.append(len(copies))
        for j in range(local):
            for i in range(3):
                weight_copy(i, j).start()
        before = (
            lax.broadcasted_iota(jnp.int32, (tok_rows, tok_rows), 0)
            < lax.broadcasted_iota(jnp.int32, (tok_rows, tok_rows), 1)
        )
        before = jnp.where(before, 1.0, 0.0).astype(bf16)
        slot = lax.broadcasted_iota(jnp.int32, (cap, tok_rows), 0).astype(f32)
        out_part, in_part = dense_w_ref.shape[1], dense_w_ref.shape[0]
        own_cols = pl.ds(pl.multiple_of(tp * in_part, 128), in_part)
        out_cols = pl.ds(pl.multiple_of(ep * out_part, 128), out_part)
        dense_sum = jnp.zeros(dgrad_ref.shape, f32) if fresh else dgrad_in[...]
        for b in range(count):
            for copy in copies[counts[b] : counts[b + 1]]:
                copy.wait()
            for j in range(local):
                chosen = table(b, ep * local + j)[1]
                rank = jnp.dot(
                    jnp.broadcast_to(chosen, (8, tok_rows)).astype(bf16),
                    before,
                    preferred_element_type=f32,
                )[:1]
                place = jnp.where(chosen > 0.0, rank, -1.0)
                picks[b, j * cap : (j + 1) * cap] = jnp.where(slot == place, 1.0, 0.0).astype(bf16)
            for which, out in ((0, rows_s), (1, cots_s)):
                for low in range(0, width, step):
                    got = jnp.dot(
                        picks[b], block[b, which, :, low : low + step],
                        preferred_element_type=f32,
                    ).astype(bf16)
                    for j in range(local):
                        out[j, b * cap : (b + 1) * cap, low : low + step] = got[
                            j * cap : (j + 1) * cap
                        ]
            gated = (dense_g_ref[:, out_cols] * block[b, 1, :, out_cols].astype(f32)).astype(bf16)
            dense[b] = columns(gated, dense_w_ref[...])
            dense_sum = dense_sum + outer(block[b, 0, :, own_cols], gated)
        dgrad_ref[...] = dense_sum
        score_total[...] = jnp.zeros_like(score_total)

    for i in range(3):
        weight_copy(i, e).wait()
    rows, cots = rows_s[e], cots_s[e]
    row_ref[0] = rows
    own_rows = pl.ds(pl.multiple_of(e * cap, 16), cap)
    own_picks = [picks[b, own_rows] for b in range(count)]
    tables = [table(b, ep * local + e) for b in range(count)]
    scale = jnp.concatenate(
        [
            jnp.sum(own_picks[b].astype(f32) * tables[b][2], axis=1, keepdims=True)
            for b in range(count)
        ],
        axis=0,
    )
    gate_pre = jnp.dot(rows, wg_ref[e], preferred_element_type=f32)
    up_pre = jnp.dot(rows, wu_ref[e], preferred_element_type=f32)
    down_back = columns(cots, wd_ref[e])
    gate_val = jnp.minimum(gate_pre, clamp_limit)
    up_val = jnp.clip(up_pre, -clamp_limit, clamp_limit)
    squash = jax.nn.sigmoid(sigmoid_slope * gate_val)
    hidden = ((up_val + 1.0) * gate_val * squash).astype(bf16)
    product = hidden.astype(f32) * down_back
    hidden_back = scale * down_back
    gate_slope = squash + sigmoid_slope * gate_val * squash * (1.0 - squash)
    gate_back = jnp.where(
        gate_pre < clamp_limit, hidden_back * (up_val + 1.0) * gate_slope, 0.0
    ).astype(bf16)
    up_back = jnp.where(
        jnp.abs(up_pre) < clamp_limit, hidden_back * gate_val * squash, 0.0
    ).astype(bf16)
    hid_ref[0], gb_ref[0], ub_ref[0] = hidden, gate_back, up_back
    wt_ref[0] = (scale * cots.astype(f32)).astype(bf16)
    for low in range(0, width, step):
        cols = slice(low, low + step)
        value = (
            columns(gate_back, wg_ref[e, cols]) + columns(up_back, wu_ref[e, cols])
        ).astype(bf16)
        for b in range(count):
            back[b, own_rows, cols] = value[b * cap : (b + 1) * cap]
    score = jnp.sum(product, axis=1, keepdims=True)
    for b in range(count):
        by_token = jnp.sum(
            own_picks[b].astype(f32) * score[b * cap : (b + 1) * cap], axis=0, keepdims=True
        )
        score_total[b, :top] += tables[b][0] * by_token

    @pl.when(e == local - 1)
    def _():
        part = dense.shape[2]
        for b in range(count):
            for p in range(tp_size):
                out = send_ref if p % 2 else keep_ref
                cols = pl.ds(pl.multiple_of((tp ^ p) * part, 128), part)
                value = outer(picks[b], back[b, :, cols])
                if p == 0:
                    value = value + dense[b]
                out[b, p // 2, :tok_rows] = value.astype(bf16)
                out[b, p // 2, tok_rows:] = jnp.zeros((out.shape[2] - tok_rows, part), bf16)
                out[b, p // 2, tok_rows:, :tok_rows] = score_total[b].astype(bf16)


def expert_pair(
    blocks, weights, dense_w, dense_g, dgrad, slabs, first, count_all, tok_rows, cap, top
):
    local, width, units = weights[0].shape
    count = len(blocks)
    part = dense_w.shape[0]
    halves = lax.axis_size("tp") // 2
    m = count * cap
    vmem = pl.BlockSpec(memory_space=pltpu.VMEM)
    hbm = pl.BlockSpec(memory_space=pltpu.HBM)
    arrays = [v for values, _ in blocks for v in values]
    layout = tuple((len(values), masks) for values, masks in blocks)
    payload = jax.ShapeDtypeStruct((count, halves, tok_rows + 8, part), bf16)
    window = lambda lanes: pl.BlockSpec((1, m, lanes), lambda e: (e, first // count, 0))
    slab_lanes = (width, units, units, units, width)
    operands = [*arrays, *weights, dense_w, dense_g]
    specs = [hbm] * (len(arrays) + 3) + [vmem] * 2
    aliases = {}
    if slabs is not None:
        aliases = {len(operands) + 1 + i: i for i in range(5)}
        operands += [dgrad, *slabs]
        specs += [vmem] + [hbm] * 5
    return pl.pallas_call(
        functools.partial(pair_kernel, layout, local, cap, slabs is None),
        grid=(local,),
        out_shape=(
            *[jax.ShapeDtypeStruct((local, count_all * cap, n), bf16) for n in slab_lanes],
            payload,
            payload,
            jax.ShapeDtypeStruct(dense_w.shape, f32),
        ),
        in_specs=specs,
        out_specs=(*[window(n) for n in slab_lanes], vmem, vmem, vmem),
        scratch_shapes=[
            *[pltpu.VMEM(w.shape, bf16) for w in weights],
            pltpu.SemaphoreType.DMA((3, local)),
            pltpu.VMEM((count, 2, tok_rows, width), bf16),
            pltpu.VMEM((count, 2 * top, tok_rows), bf16),
            pltpu.VMEM((count, local * cap, tok_rows), bf16),
            pltpu.VMEM((local, m, width), bf16),
            pltpu.VMEM((local, m, width), bf16),
            pltpu.VMEM((count, local * cap, width), bf16),
            pltpu.VMEM((count, tok_rows, part), f32),
            pltpu.VMEM((count, 8, tok_rows), f32),
            pltpu.SemaphoreType.DMA((3 * len(arrays),)),
        ],
        input_output_aliases=aliases,
        compiler_params=pltpu.CompilerParams(vmem_limit_bytes=56 << 20),
        cost_estimate=pl.CostEstimate(
            flops=14 * local * m * width * units,
            bytes_accessed=10 * local * width * units,
            transcendentals=local * m * units,
        ),
        name="expert_pair",
    )(*operands)


def groups_of(ep_size, halves):
    if ep_size == 8 and halves == 2:
        return ((0, 1, 2), 0), ((3, 4, 5), 3), ((6, 7), 6)
    return tuple(((b, b + 1), b) for b in range(0, ep_size, 2))


def batched(lhs, rhs):
    return lax.dot_general(lhs, rhs, (((1,), (1,)), ((0,), (0,))), preferred_element_type=f32)


def shards(
    tokens,
    cotangent,
    expert_ids,
    route_weights,
    gate_weight,
    up_weight,
    down_weight,
    dense_weight,
    dense_gate,
):
    tok_rows, width = tokens.shape
    top_count = expert_ids.shape[1]
    local = gate_weight.shape[0]
    ep_size = lax.axis_size("ep")
    tp_size = lax.axis_size("tp")
    ep, tp = lax.axis_index("ep"), lax.axis_index("tp")
    cap = tok_rows * top_count * 3 // (2 * local * ep_size)
    halves = tp_size // 2
    quarter_rows = tok_rows // tp_size
    half_rows = tok_rows // 2

    meta = jnp.concatenate([expert_ids.T.astype(bf16), route_weights.T], axis=0)
    meta_rows = jnp.pad(meta, ((0, 0), (0, width - tok_rows)))

    def share(start, rows):
        return jnp.concatenate(
            [
                lax.dynamic_slice_in_dim(tokens, start, rows, 0),
                lax.dynamic_slice_in_dim(cotangent, start, rows, 0),
                meta_rows,
            ],
            axis=0,
        )

    own_half = share((tp % 2) * half_rows, half_rows)
    own_quarter = share(((tp % 2) * halves + tp // 2) * quarter_rows, quarter_rows)
    pairs = ep_size // 2
    line = pairs == 4 and halves == 2
    middle = (ep // 2 == 1) | (ep // 2 == 2)

    def along(value, moves):
        return lax.ppermute(
            value, "ep", [(2 * a + i, 2 * b + i) for a, b in moves for i in range(2)]
        )

    far = [None] * pairs
    if line:
        far[1] = along(own_quarter, ((0, 1), (1, 0), (2, 3), (3, 2)))
        inner = along(own_quarter, ((1, 2), (2, 1)))
        far[2] = jnp.where(middle, inner, along(inner, ((1, 0), (2, 3))))
        inner = along(far[1], ((1, 2), (2, 1)))
        far[3] = jnp.where(middle, inner, along(inner, ((1, 0), (2, 3))))
    else:
        for k in range(1, pairs):
            far[k] = swap(own_quarter, "ep", 2 * k)
    near = [swap(own_half, "ep", 1)]
    near += [swap(far[k], "ep", 1) for k in range(1, pairs)]

    def gathered(value, whole):
        held = [(value, 0)]
        if not whole:
            held += [(swap(value, "tp", 2 * p), 2 * p) for p in range(1, halves)]
        held += [(swap(v, "tp", 1), mask ^ 1) for v, mask in tuple(held)]
        return [v for v, _ in held], tuple(mask for _, mask in held)

    blocks = [[([tokens, cotangent, meta], None), gathered(near[0], True)]]
    for k in range(1, pairs):
        blocks.append([gathered(far[k], False), gathered(near[k], False)])

    dense_g = dense_gate[None, :]
    dgrad = None
    weights = (gate_weight, up_weight, down_weight)
    slabs = None
    results, summed = {}, {}
    flat = [block for pair in blocks for block in pair]
    for members, first in groups_of(ep_size, halves):
        *slabs, keep, send, dgrad = expert_pair(
            [flat[b] for b in members], weights, dense_weight, dense_g, dgrad, slabs, first,
            ep_size, tok_rows, cap, top_count,
        )
        other = swap(send, "tp", 1)
        held = [(keep[i].astype(f32) + other[i].astype(f32)).astype(bf16) for i in range(len(members))]
        summed.update(zip(members, lax.optimization_barrier(held)))
    for k in range(pairs):
        moved = swap(summed[2 * k + 1], "ep", 1)
        both = summed[2 * k].astype(f32) + moved.astype(f32)
        total = both[0]
        for h in range(1, halves):
            total = total + swap(both[h].astype(bf16), "tp", 2 * h).astype(f32)
        results[k] = total
    row, hid, gb, ub, wt = slabs
    grads = []
    for left, right in ((row, gb), (row, ub), (hid, wt)):
        grads.append(batched(left, right))
    grad_gate, grad_up, grad_down = grads

    total = results[0]
    for k in range(1, pairs):
        value = results[k].astype(bf16)
        if not line or k == 1:
            total = total + swap(value, "ep", 2 * k).astype(f32)
            continue
        straight, crossed = ((0, 2), (3, 1)), ((1, 2), (2, 1))
        if k == 3:
            straight, crossed = ((1, 3), (2, 0)), ((0, 3), (3, 0))
        total = total + along(value, straight).astype(f32)
        total = total + along(value, crossed).astype(f32)
    token_grad = total[:tok_rows].astype(bf16)
    weight_grad = total[tok_rows : tok_rows + top_count, :tok_rows].astype(bf16).T
    return (token_grad, weight_grad, grad_gate, grad_up, grad_down, dgrad)


def solution(mesh):
    in_specs = (
        P("ep", None),
        P("ep", None),
        P("ep", None),
        P("ep", None),
        P("ep", None, "tp"),
        P("ep", None, "tp"),
        P("ep", "tp", None),
        P("tp", "ep"),
        P(),
    )
    out_specs = (
        P("ep", "tp"),
        P("ep", None),
        P("ep", None, "tp"),
        P("ep", None, "tp"),
        P("ep", "tp", None),
        P("tp", "ep"),
    )

    return jax.shard_map(shards, mesh=mesh, in_specs=in_specs, out_specs=out_specs, check_vma=False)
```
